32 devices in a mesh: sp: 16 (over z, y, x), tp: 2 (over core).
Axes of the slice: x: 2, y: 2, z: 4, core: 2. Of those that a mesh axis runs over, the one named last changes fastest.
Arguments:
- stream: bfloat16 [4096, 2048], P(('sp', 'tp')), may hold values from -6 to 6
- head_input_signal: bfloat16 [4096, 2048], P('sp', 'tp'), may hold values from -6 to 6
- write_input_vectors: bfloat16 [4096, 512], P('sp', 'tp'), may hold values from -6 to 6
- read_input_vectors: bfloat16 [4096, 512], P('sp', 'tp'), may hold values from -6 to 6
- output_gate_input: bfloat16 [4096, 2048], P('sp', 'tp'), may hold values from -6 to 6
- step_size_input: bfloat16 [4096, 32], P('sp', 'tp'), may hold values from -5 to 5.5
- position_log_decay: float32 [4096, 32], P('sp', 'tp'), may hold values from -0.7 to 0
- signal_filter_taps: bfloat16 [4, 2048], P(None, 'tp'), may hold values from -3 to 3
- write_filter_taps: bfloat16 [4, 512], P(None, 'tp'), may hold values from -3 to 3
- read_filter_taps: bfloat16 [4, 512], P(None, 'tp'), may hold values from -3 to 3
- step_size_bias: float32 [32], P('tp'), may hold values from -1 to 1
- head_decay_rate: float32 [32], P('tp'), may hold values from 2.4414063e-06 to 0.03
- head_direct_term: float32 [32], P('tp'), may hold values from 0.5 to 2
- grouped_norm_gain: float32 [2048], P('tp'), may hold values from 0.1 to 1.9
- mixer_output_weight: bfloat16 [2048, 2048], P('tp'), may hold values from -0.125 to 0.125
- expert_norm_gain: float32 [2048], replicated, may hold values from 0.1 to 1.9
- chosen_expert_index: int32 [4096, 4], P(('sp', 'tp')), may hold values from 0 to 31, all different within a row; in each aligned block of 128 rows (0 to 127, 128 to 255, ...) at most 24 rows name the same one
- chosen_expert_weight: float32 [4096, 4], P(('sp', 'tp')), may hold values from 0.1 to 1
- routed_gate_weight: bfloat16 [32, 2048, 512], P(('sp', 'tp')), may hold values from -0.125 to 0.125
- routed_up_weight: bfloat16 [32, 2048, 512], P(('sp', 'tp')), may hold values from -0.125 to 0.125
- routed_down_weight: bfloat16 [32, 512, 2048], P(('sp', 'tp')), may hold values from -0.25 to 0.25
- common_gate_weight: bfloat16 [2048, 512], replicated, may hold values from -0.125 to 0.125
- common_up_weight: bfloat16 [2048, 512], replicated, may hold values from -0.125 to 0.125
- common_down_weight: bfloat16 [512, 2048], replicated, may hold values from -0.25 to 0.25
Outputs:
- layer_out: bfloat16 [4096, 2048], P(('sp', 'tp'))
The draws below stay inside these ranges and needn't reach their ends.
Inputs may be any that keep to these rules, and one draw needn't show every extreme that they name: `chosen_expert_index`: each row names 4 different experts. Among the 128 rows of one device (aligned blocks of 128 rows) no expert is named more than 24 times; in some block one expert is named exactly 24 times.
All inputs are finite; a program needn't handle non-finite values.
Results may differ from the reference program's by a relative error of at most 0.015.
Values may be sent and summed in bfloat16 or wider, within the bound.
A program may use at most 128 MiB of HBM per device.

```python
import math
import jax
import jax.numpy as jnp
import numpy as np
from jax import lax

D = 2048
HEADS = 32
HEAD_DIM = 64
GROUPS = 4
STATE = 128
CONV_K = 4
BLK = 128
EFF = 512
SFF = 512
TOP = 4
TOK_DEV = 256
SSM_WIDTH = 2048
TOKENS = 4096
ROWS = 128
EXPERTS = 32
CAP = 24
N_SP = 16
N_TP = 2


def draw_step_size_input(key, part):
    first_key, second_key = jax.random.split(jax.random.fold_in(key, 11))
    base = jnp.clip(jax.random.normal(first_key, (TOKENS, HEADS), jnp.float32), -4.0, 4.0)
    shifts = jax.random.uniform(second_key, (TOKENS // TOK_DEV, 1, 1), jnp.float32, -1.0, 1.5)
    shifts = jnp.broadcast_to(shifts, (TOKENS // TOK_DEV, TOK_DEV, HEADS)).reshape(TOKENS, HEADS)
    return (base + shifts).astype(jnp.bfloat16)


def draw_position_log_decay(key, part):
    first_key, second_key = jax.random.split(jax.random.fold_in(key, 23))
    spots = jax.random.randint(first_key, (8,), 0, TOKENS)
    struck = jnp.any(jnp.arange(TOKENS)[:, None] == spots[None, :], axis=1)
    values = jax.random.uniform(second_key, (TOKENS, HEADS), jnp.float32, -0.69, -0.22)
    return jnp.where(struck[:, None], values, 0.0).astype(jnp.float32)


def draw_head_decay_rate(key, part):
    lowest = math.log(0.01 / TOKENS)
    highest = math.log(0.03)
    logs = jax.random.uniform(jax.random.fold_in(key, 37), (HEADS,), jnp.float32, lowest, highest)
    return jnp.exp(logs).astype(jnp.float32)


def block_scale(key, dims, shards, smallest, top_value):
    factor_of, own = 1.0, jax.random.fold_in(key, 6)
    for axis_at, blocks in shards:
        heights = jnp.exp(jax.random.uniform(jax.random.fold_in(own, axis_at), (blocks,), jnp.float32, smallest / len(shards), top_value / len(shards)))
        factor_of = factor_of * jnp.repeat(heights, dims[axis_at] // blocks).reshape([-1 if axis == axis_at else 1 for axis in range(len(dims))])
    return factor_of


def routed_block(stream_key, own, number, rows, number_of, top, bound, lean):
    order = jax.random.permutation(stream_key, number_of)
    packed, ordinary = shares(number_of, rows * top, bound, lean, True), shares(number_of, rows * top, bound, lean, False)
    places = jnp.arange(number_of)

    def named(tallies, turn):
        used = int((tallies > 0).sum())
        fixed = max(1, used // 4)
        shifted = fixed + (places - fixed + turn * (used - fixed)) % max(1, number_of - fixed)
        return jnp.zeros((number_of,), jnp.int32).at[order[jnp.where(places < fixed, places, shifted)]].set(jnp.asarray(tallies, jnp.int32))

    tallies = jnp.where(number % 4 == 0, named(packed, number // 4), named(ordinary, number - number // 4 - 1))
    mixed = jax.random.permutation(jax.random.fold_in(own, 3), number_of)
    giver, sink = mixed[0:number_of // 2 * 2:2], mixed[1:number_of // 2 * 2:2]
    room = jnp.minimum(tallies[giver] - 1, bound - tallies[sink]) // 2
    room = jnp.where((giver == order[0]) | (sink == order[0]) | (tallies[sink] == 0), 0, jnp.maximum(room, 0))
    shifted = jax.random.randint(jax.random.fold_in(own, 4), (number_of // 2,), 0, 1 << 20) % (room + 1)
    tallies = tallies.at[giver].add(-shifted).at[sink].add(shifted)
    members = jnp.searchsorted(jnp.cumsum(tallies), jnp.arange(rows * top), side="right").astype(jnp.int32)
    table = members.reshape(top, rows).T
    table = table[jax.random.permutation(jax.random.fold_in(own, 1), rows)]
    turn = jax.random.randint(jax.random.fold_in(own, 2), (rows, 1), 0, top)
    return jnp.take_along_axis(table, (jnp.arange(top)[None, :] + turn) % top, axis=1)


def shares(amount, total, limit, slope, full):
    loads = [(1 << 20) // math.isqrt(standing ** slope) + 1 for standing in range(1, amount + 1)]
    largest = limit if full else min(limit, max(-(-total // amount), total * loads[0] // sum(loads)))
    least = 1 if total - largest >= amount - 1 else 0
    given, rest = [largest] + [least] * (amount - 1), total - largest - least * (amount - 1)
    while rest > 0:
        free = [i for i in range(1, amount) if given[i] < largest] or [i for i in range(1, amount) if given[i] < limit]
        pool, budget = sum([loads[i] for i in free]), rest
        for i in free:
            more = min(limit - given[i], max(1, budget * loads[i] // pool), rest)
            given[i] = given[i] + more
            rest = rest - more
    return np.array(given)


def scatter_about(stream_key, extent, deviation, reach, cuts=(), kind=jnp.bfloat16):
    loudness = block_scale(stream_key, extent, cuts, -0.22, 0.18) if cuts else 1.0
    drawn = jax.random.normal(stream_key, extent, jnp.float32) * deviation * loudness
    return jnp.minimum(jnp.maximum(drawn, -reach), reach).astype(kind)


def setup_inputs(seed: int = 0) -> dict:
    arg_keys = jax.random.split(jax.random.key(seed), 25)
    stream = scatter_about(arg_keys[0], (TOKENS, D), 1.0, 6.0, ((0, 32),))
    head_input_signal = scatter_about(arg_keys[1], (TOKENS, SSM_WIDTH), 1.0, 6.0, ((0, 16), (1, 2)))
    write_input_vectors = scatter_about(arg_keys[2], (TOKENS, GROUPS * STATE), 1.0, 6.0, ((0, 16), (1, 2)))
    read_input_vectors = scatter_about(arg_keys[3], (TOKENS, GROUPS * STATE), 1.0, 6.0, ((0, 16), (1, 2)))
    output_gate_input = scatter_about(arg_keys[4], (TOKENS, SSM_WIDTH), 1.0, 6.0, ((0, 16), (1, 2)))
    step_size_input = draw_step_size_input(jax.random.fold_in(arg_keys[24], 71), 0)
    position_log_decay = draw_position_log_decay(jax.random.fold_in(arg_keys[24], 71), 0)
    signal_filter_taps = scatter_about(arg_keys[7], (CONV_K, SSM_WIDTH), CONV_K ** -0.5, 3.0, ((1, 2),))
    write_filter_taps = scatter_about(arg_keys[8], (CONV_K, GROUPS * STATE), CONV_K ** -0.5, 3.0, ((1, 2),))
    read_filter_taps = scatter_about(arg_keys[9], (CONV_K, GROUPS * STATE), CONV_K ** -0.5, 3.0, ((1, 2),))
    step_size_bias = jnp.clip(jax.random.uniform(arg_keys[10], (HEADS,), jnp.float32, -1.0, 1.0) * block_scale(arg_keys[10], (HEADS,), ((0, 2),), -0.4, 0.0), -1.0, 1.0)
    head_decay_rate = draw_head_decay_rate(jax.random.fold_in(arg_keys[24], 71), 0)
    head_direct_term = jnp.clip(0.5 + 1.5 * jax.random.uniform(arg_keys[12], (HEADS,), jnp.float32) ** block_scale(arg_keys[12], (HEADS,), ((0, 2),), -0.2, 0.2), 0.5, 2.0)
    grouped_norm_gain = jnp.clip(1.0 + 0.18 * jax.random.normal(arg_keys[13], (SSM_WIDTH,), jnp.float32), 0.1, 1.9)
    mixer_output_weight = scatter_about(arg_keys[14], (SSM_WIDTH, D), SSM_WIDTH ** -0.5, 0.125, ((0, 2),))
    expert_norm_gain = jnp.clip(1.0 + 0.18 * jax.random.normal(arg_keys[15], (D,), jnp.float32), 0.1, 1.9)
    chosen_expert_index_keys = jax.random.split(jax.random.fold_in(arg_keys[16], 1), TOKENS // ROWS)
    chosen_expert_index_turns = jax.random.permutation(jax.random.fold_in(arg_keys[16], 3), TOKENS // ROWS)
    chosen_expert_index = jax.vmap(lambda own, number: routed_block(jax.random.fold_in(arg_keys[16], 2), own, number, ROWS, EXPERTS, TOP, CAP, 1))(chosen_expert_index_keys, chosen_expert_index_turns).reshape((TOKENS, TOP))
    chosen_expert_weight = jnp.clip(0.1 + 0.9 * jax.random.uniform(arg_keys[17], (TOKENS, TOP), jnp.float32) ** block_scale(arg_keys[17], (TOKENS, TOP), ((0, 32),), -0.2, 0.2), 0.1, 1.0)
    routed_gate_weight = scatter_about(arg_keys[18], (EXPERTS, D, EFF), D ** -0.5, 0.125, ((0, 32),))
    routed_up_weight = scatter_about(arg_keys[19], (EXPERTS, D, EFF), D ** -0.5, 0.125, ((0, 32),))
    routed_down_weight = scatter_about(arg_keys[20], (EXPERTS, EFF, D), EFF ** -0.5, 0.25, ((0, 32),))
    common_gate_weight = scatter_about(arg_keys[21], (D, SFF), D ** -0.5, 0.125)
    common_up_weight = scatter_about(arg_keys[22], (D, SFF), D ** -0.5, 0.125)
    common_down_weight = scatter_about(arg_keys[23], (SFF, D), SFF ** -0.5, 0.25)
    return {"stream": stream, "head_input_signal": head_input_signal, "write_input_vectors": write_input_vectors, "read_input_vectors": read_input_vectors, "output_gate_input": output_gate_input, "step_size_input": step_size_input, "position_log_decay": position_log_decay, "signal_filter_taps": signal_filter_taps, "write_filter_taps": write_filter_taps, "read_filter_taps": read_filter_taps, "step_size_bias": step_size_bias, "head_decay_rate": head_decay_rate, "head_direct_term": head_direct_term, "grouped_norm_gain": grouped_norm_gain, "mixer_output_weight": mixer_output_weight, "expert_norm_gain": expert_norm_gain, "chosen_expert_index": chosen_expert_index, "chosen_expert_weight": chosen_expert_weight, "routed_gate_weight": routed_gate_weight, "routed_up_weight": routed_up_weight, "routed_down_weight": routed_down_weight, "common_gate_weight": common_gate_weight, "common_up_weight": common_up_weight, "common_down_weight": common_down_weight}


precise = lax.Precision.HIGHEST

def causal_conv(previous, current, weight):
    stacked = jnp.concatenate([previous, current], axis=0).astype(jnp.float32)
    weight = weight.astype(jnp.float32)
    kernel_len = weight.shape[0]
    length = current.shape[0]
    summed_taps = weight[0] * stacked[0:length]
    for offset in range(1, kernel_len):
        summed_taps = summed_taps + weight[offset] * stacked[offset:offset + length]
    return jax.nn.silu(summed_taps)

def reference(stream, head_input_signal, write_input_vectors, read_input_vectors, output_gate_input, step_size_input, position_log_decay, signal_filter_taps, write_filter_taps, read_filter_taps, step_size_bias, head_decay_rate, head_direct_term, grouped_norm_gain, mixer_output_weight, expert_norm_gain, chosen_expert_index, chosen_expert_weight, routed_gate_weight, routed_up_weight, routed_down_weight, common_gate_weight, common_up_weight, common_down_weight):
    margin = CONV_K - 1
    signal = causal_conv(jnp.zeros((margin, SSM_WIDTH), jnp.bfloat16), head_input_signal, signal_filter_taps)
    write_vec = causal_conv(jnp.zeros((margin, GROUPS * STATE), jnp.bfloat16), write_input_vectors, write_filter_taps)
    read_vec = causal_conv(jnp.zeros((margin, GROUPS * STATE), jnp.bfloat16), read_input_vectors, read_filter_taps)
    time_position = jax.nn.softplus(step_size_input.astype(jnp.float32) + step_size_bias)
    decay_logarithm = position_log_decay - head_decay_rate * time_position
    per_group = HEADS // GROUPS
    blocks = TOKENS // BLK
    signal_heads = signal.reshape(TOKENS, GROUPS, per_group, HEAD_DIM)
    scaled_in = signal_heads * time_position.reshape(TOKENS, GROUPS, per_group)[..., None]
    causal = jnp.arange(BLK)[:, None] >= jnp.arange(BLK)[None, :]
    skip_heads = head_direct_term.reshape(GROUPS, per_group)[:, :, None]

    def advance(carry_state, inputs):
        scaled_blk, write_blk, read_blk, decay_blk, signal_blk = inputs
        within_cum = jnp.cumsum(decay_blk, axis=0)
        cum_heads = jnp.transpose(within_cum, (1, 2, 0))
        decay_matrix = jnp.exp(jnp.where(causal, cum_heads[..., :, None] - cum_heads[..., None, :], -jnp.inf))
        intersection = jnp.einsum('tgn,sgn->gts', read_blk, write_blk, precision=precise)
        intra = jnp.einsum('gts,gets,sgep->tgep', intersection, decay_matrix, scaled_blk, precision=precise)
        carried = jnp.einsum('tgn,gepn,tge->tgep', read_blk, carry_state, jnp.exp(within_cum), precision=precise)
        tail_decay = jnp.exp(within_cum[-1][None] - within_cum)
        fresh = jnp.einsum('sgn,sge,sgep->gepn', write_blk, tail_decay, scaled_blk, precision=precise)
        next_state = carry_state * jnp.exp(within_cum[-1])[..., None, None] + fresh
        return (next_state, intra + carried + skip_heads * signal_blk)
    sequence = (scaled_in.reshape(blocks, BLK, GROUPS, per_group, HEAD_DIM), write_vec.reshape(blocks, BLK, GROUPS, STATE), read_vec.reshape(blocks, BLK, GROUPS, STATE), decay_logarithm.reshape(blocks, BLK, GROUPS, per_group), signal_heads.reshape(blocks, BLK, GROUPS, per_group, HEAD_DIM))
    initial = jnp.zeros((GROUPS, per_group, HEAD_DIM, STATE), jnp.float32)
    ssd_out = lax.scan(advance, initial, sequence)[1]
    gated = ssd_out.reshape(TOKENS, GROUPS, per_group * HEAD_DIM) * jax.nn.silu(output_gate_input.astype(jnp.float32)).reshape(TOKENS, GROUPS, per_group * HEAD_DIM)
    norm_scale = lax.rsqrt(lax.optimization_barrier(jnp.mean(gated * gated, axis=-1, keepdims=True)) + 1e-06)
    mixer_out = ((gated * norm_scale).reshape(TOKENS, SSM_WIDTH) * grouped_norm_gain).astype(jnp.bfloat16)
    residual = (stream.astype(jnp.float32) + jnp.dot(mixer_out, mixer_output_weight, preferred_element_type=jnp.float32)).astype(jnp.bfloat16)
    widened = residual.astype(jnp.float32)
    normed = (widened * lax.rsqrt(lax.optimization_barrier(jnp.mean(widened * widened, axis=-1, keepdims=True)) + 1e-06) * expert_norm_gain).astype(jnp.bfloat16)
    shared_hidden = (jax.nn.silu(jnp.dot(normed, common_gate_weight, preferred_element_type=jnp.float32)) * jnp.dot(normed, common_up_weight, preferred_element_type=jnp.float32)).astype(jnp.bfloat16)
    shared = jnp.dot(shared_hidden, common_down_weight, preferred_element_type=jnp.float32)
    row_total = TOKENS * TOP
    chosen = chosen_expert_index.reshape(-1).astype(jnp.int32)
    one_hot = (chosen[:, None] == jnp.arange(EXPERTS, dtype=jnp.int32)[None, :]).astype(jnp.int32)
    slot_index = lax.optimization_barrier(jnp.sum((jnp.cumsum(one_hot, axis=0) - one_hot) * one_hot, axis=1)).astype(jnp.int32)
    slot_limit = N_SP * N_TP * CAP
    source_row = (jnp.arange(row_total, dtype=jnp.int32) // TOP).astype(jnp.int32)
    slot_table = jnp.full((EXPERTS, slot_limit), TOKENS, jnp.int32).at[chosen, slot_index].set(source_row)
    weight_table = jnp.zeros((EXPERTS, slot_limit), jnp.float32).at[chosen, slot_index].set(chosen_expert_weight.reshape(-1))
    padded = jnp.concatenate([normed, jnp.zeros((1, D), normed.dtype)], axis=0)

    def serve_expert(summed, inputs):
        gate_w, up_w, down_w, indices, weights = inputs
        picked = padded[indices]
        hidden = (jax.nn.silu(jnp.dot(picked, gate_w, preferred_element_type=jnp.float32)) * jnp.dot(picked, up_w, preferred_element_type=jnp.float32)).astype(jnp.bfloat16)
        result = jnp.dot(hidden, down_w, preferred_element_type=jnp.float32).astype(jnp.bfloat16)
        return (summed.at[indices].add(weights[:, None] * result.astype(jnp.float32), mode='drop'), None)
    routed = lax.scan(serve_expert, jnp.zeros((TOKENS, D), jnp.float32), (routed_gate_weight, routed_up_weight, routed_down_weight, slot_table, weight_table))[0]
    return (widened + shared + routed).astype(jnp.bfloat16)
```

```python
import jax
import jax.numpy as jnp
from jax import lax
from jax.sharding import PartitionSpec as P

HEAD_DIM = 64
STATE = 128
BLK = 128


def from_behind(block, axis, distance):
    devices = range(lax.axis_size(axis))
    route = [(i - distance, i) for i in devices if i - distance in devices]
    return lax.ppermute(block, axis, route)


def swap(block, axis, step, upward_only):
    devices = range(lax.axis_size(axis))
    route = [(i, i ^ step) for i in devices if not (upward_only and i & step)]
    return lax.ppermute(block, axis, route)


def carried_in(log_total, state, axis):
    count, mine = lax.axis_size(axis), lax.axis_index(axis)
    heads, width = log_total.size, state.shape[-1]
    flat = state.reshape(heads, -1, width)
    decay = jnp.exp(log_total).reshape(heads)
    total, before, before_decay = flat, jnp.zeros_like(flat), jnp.ones_like(decay)
    step = 1
    while step < count:
        coarse = lax.reduce_precision(decay, 8, 7)
        lane = jnp.arange(width)[None, :]
        tail = jnp.where(lane == 0, coarse[:, None], jnp.where(lane == 1, (decay - coarse)[:, None], 0.0))
        sent = jnp.concatenate([total.reshape(-1, width), tail], axis=0).astype(jnp.bfloat16)
        got = swap(sent, axis, step, 2 * step >= count).astype(jnp.float32)
        other = got[: got.shape[0] - heads].reshape(flat.shape)
        other_decay = got[got.shape[0] - heads :, 0] + got[got.shape[0] - heads :, 1]
        upper = (mine & step) != 0
        before = before + jnp.where(upper, before_decay, 0.0)[:, None, None] * other
        if 2 * step < count:
            before_decay = before_decay * jnp.where(upper, other_decay, 1.0)
            total = jnp.where(
                upper, other * decay[:, None, None] + total, total * other_decay[:, None, None] + other
            )
            decay = decay * other_decay
        step *= 2
    return before.reshape(state.shape)


def causal_conv(previous, current, weight):
    stacked = jnp.concatenate([previous, current], axis=0).astype(jnp.float32)
    weight = weight.astype(jnp.float32)
    kernel_len = weight.shape[0]
    length = current.shape[0]
    summed_taps = weight[0] * stacked[0:length]
    for offset in range(1, kernel_len):
        summed_taps = summed_taps + weight[offset] * stacked[offset : offset + length]
    return jax.nn.silu(summed_taps)


def product(spec, *operands):
    return jnp.einsum(
        spec, *[part.astype(jnp.bfloat16) for part in operands], preferred_element_type=jnp.float32
    )


def on_device(
    stream,
    head_input_signal,
    write_input_vectors,
    read_input_vectors,
    output_gate_input,
    step_size_input,
    position_log_decay,
    signal_filter_taps,
    write_filter_taps,
    read_filter_taps,
    step_size_bias,
    head_decay_rate,
    head_direct_term,
    grouped_norm_gain,
    mixer_output_weight,
    expert_norm_gain,
    chosen_expert_index,
    chosen_expert_weight,
    routed_gate_weight,
    routed_up_weight,
    routed_down_weight,
    common_gate_weight,
    common_up_weight,
    common_down_weight,
):
    length = head_input_signal.shape[0]
    margin = signal_filter_taps.shape[0] - 1
    head_count = step_size_input.shape[1]
    groups = write_input_vectors.shape[1] // STATE
    per_group = head_count // groups
    blocks = length // BLK
    wide, narrow = head_input_signal.shape[1], write_input_vectors.shape[1]
    rim = jnp.concatenate(
        [part[length - margin :] for part in (head_input_signal, write_input_vectors, read_input_vectors)],
        axis=1,
    )
    rim = from_behind(rim, "sp", 1)
    before = (rim[:, :wide], rim[:, wide : wide + narrow], rim[:, wide + narrow :])
    signal = causal_conv(before[0], head_input_signal, signal_filter_taps)
    write_vec = causal_conv(before[1], write_input_vectors, write_filter_taps)
    read_vec = causal_conv(before[2], read_input_vectors, read_filter_taps)
    time_position = jax.nn.softplus(step_size_input.astype(jnp.float32) + step_size_bias)
    decay_logarithm = position_log_decay - head_decay_rate * time_position
    signal_heads = signal.reshape(blocks, BLK, groups, per_group, HEAD_DIM)
    scaled_blocks = signal_heads * time_position.reshape(blocks, BLK, groups, per_group)[..., None]
    write_blocks = write_vec.reshape(blocks, BLK, groups, STATE)
    read_blocks = read_vec.reshape(blocks, BLK, groups, STATE)
    within_cum = jnp.cumsum(decay_logarithm.reshape(blocks, BLK, groups, per_group), axis=1)
    block_total = within_cum[:, -1]
    running = jnp.cumsum(block_total, axis=0)
    device_total = running[-1]
    causal = jnp.arange(BLK)[:, None] >= jnp.arange(BLK)[None, :]
    cum_heads = jnp.transpose(within_cum, (0, 2, 3, 1))
    differences = cum_heads[..., :, None] - cum_heads[..., None, :]
    decay_matrix = jnp.exp(jnp.where(causal, differences, -jnp.inf))
    tail_decay = jnp.exp(block_total[:, None] - within_cum)
    block_states = product(
        "bsgn,bsgep->bgepn", write_blocks, scaled_blocks * tail_decay[..., None]
    )
    device_state = jnp.sum(
        block_states * jnp.exp(device_total[None] - running)[..., None, None], axis=0
    )
    incoming = carried_in(device_total, device_state, "sp")
    intersection = product("btgn,bsgn->bgts", read_blocks, write_blocks)
    intra_out = product(
        "bgets,bsgep->btgep", intersection[:, :, None] * decay_matrix, scaled_blocks
    )
    readout_scale = jnp.exp(within_cum)
    starts = [incoming]
    for block in range(blocks - 1):
        starts.append(
            starts[-1] * jnp.exp(block_total[block])[..., None, None] + block_states[block]
        )
    near_out = (
        product("btgn,bgepn->btgep", read_blocks, jnp.stack(starts)) * readout_scale[..., None]
    )
    ssd_out = intra_out + near_out
    ssd_out = ssd_out + head_direct_term.reshape(groups, per_group)[:, :, None] * signal_heads
    gated = ssd_out.reshape(length, groups, per_group * HEAD_DIM) * jax.nn.silu(
        output_gate_input.astype(jnp.float32)
    ).reshape(length, groups, per_group * HEAD_DIM)
    norm_scale = lax.rsqrt(jnp.mean(gated * gated, axis=-1, keepdims=True) + 1e-06)
    mixer_out = ((gated * norm_scale).reshape(length, -1) * grouped_norm_gain).astype(jnp.bfloat16)
    row_count = stream.shape[0]
    summed = lax.psum_scatter(
        jnp.dot(mixer_out, mixer_output_weight, preferred_element_type=jnp.float32).astype(
            jnp.bfloat16
        ),
        "tp",
        scatter_dimension=0,
        tiled=True,
    ).astype(jnp.float32)
    residual = (stream.astype(jnp.float32) + summed).astype(jnp.bfloat16)
    widened = residual.astype(jnp.float32)
    normed = (
        widened
        * lax.rsqrt(jnp.mean(widened * widened, axis=-1, keepdims=True) + 1e-06)
        * expert_norm_gain
    ).astype(jnp.bfloat16)
    shared_hidden = (
        jax.nn.silu(jnp.dot(normed, common_gate_weight, preferred_element_type=jnp.float32))
        * jnp.dot(normed, common_up_weight, preferred_element_type=jnp.float32)
    ).astype(jnp.bfloat16)
    shared = jnp.dot(shared_hidden, common_down_weight, preferred_element_type=jnp.float32)
    sp_count = lax.axis_size("sp")
    tp_count = lax.axis_size("tp")
    experts = sp_count * tp_count
    fanout = chosen_expert_index.shape[1]
    capacity = max(2, (3 * row_count * fanout + 2 * experts - 1) // (2 * experts))
    named = chosen_expert_index[:, :, None] == jnp.arange(experts, dtype=jnp.int32)
    hits = jnp.any(named, axis=1)
    share = jnp.sum(jnp.where(named, chosen_expert_weight[:, :, None], 0.0), axis=1)
    ahead = (jnp.arange(row_count)[:, None] > jnp.arange(row_count)[None, :]).astype(jnp.bfloat16)
    slot = jnp.dot(ahead, hits.astype(jnp.bfloat16), preferred_element_type=jnp.float32)
    slot = jnp.where(hits, slot.astype(jnp.int32), -1)
    places = jnp.arange(capacity, dtype=jnp.int32)
    pick = (slot.T[:, None, :] == places[None, :, None]).reshape(experts * capacity, row_count)
    outgoing = jnp.dot(
        pick.astype(jnp.bfloat16), normed, preferred_element_type=jnp.float32
    ).astype(jnp.bfloat16).reshape(experts, capacity, -1)
    arrived = lax.all_to_all(outgoing, ("sp", "tp"), split_axis=0, concat_axis=0, tiled=True)
    flat_rows = arrived.reshape(-1, arrived.shape[-1])
    hidden = (
        jax.nn.silu(jnp.dot(flat_rows, routed_gate_weight[0], preferred_element_type=jnp.float32))
        * jnp.dot(flat_rows, routed_up_weight[0], preferred_element_type=jnp.float32)
    ).astype(jnp.bfloat16)
    returned = lax.all_to_all(
        jnp.dot(hidden, routed_down_weight[0], preferred_element_type=jnp.float32)
        .astype(jnp.bfloat16)
        .reshape(arrived.shape),
        ("sp", "tp"),
        split_axis=0,
        concat_axis=0,
        tiled=True,
    )
    spread = jnp.where(slot[:, :, None] == places, share[:, :, None], 0.0)
    spread = spread.reshape(row_count, experts * capacity)
    coarse = lax.reduce_precision(spread, 8, 7)
    back = returned.reshape(experts * capacity, -1)
    routed = jnp.dot(
        coarse.astype(jnp.bfloat16), back, preferred_element_type=jnp.float32
    ) + jnp.dot((spread - coarse).astype(jnp.bfloat16), back, preferred_element_type=jnp.float32)
    return (widened + shared + routed).astype(jnp.bfloat16)


def solution(mesh):
    in_specs = (
        P(("sp", "tp"), None),
        P("sp", "tp"),
        P("sp", "tp"),
        P("sp", "tp"),
        P("sp", "tp"),
        P("sp", "tp"),
        P("sp", "tp"),
        P(None, "tp"),
        P(None, "tp"),
        P(None, "tp"),
        P("tp"),
        P("tp"),
        P("tp"),
        P("tp"),
        P("tp", None),
        P(),
        P(("sp", "tp"), None),
        P(("sp", "tp"), None),
        P(("sp", "tp"), None, None),
        P(("sp", "tp"), None, None),
        P(("sp", "tp"), None, None),
        P(),
        P(),
        P(),
    )
    out_specs = P(("sp", "tp"), None)
    return jax.shard_map(
        on_device, mesh=mesh, in_specs=in_specs, out_specs=out_specs, check_vma=False
    )
```

```python
import jax
import jax.numpy as jnp
from jax import lax
from jax.sharding import PartitionSpec as P

HEAD_DIM = 64
STATE = 128
BLK = 128


def from_behind(block, axis, distance):
    devices = range(lax.axis_size(axis))
    route = [(i - distance, i) for i in devices if i - distance in devices]
    return lax.ppermute(block, axis, route)


def swap(block, axis, step, upward_only):
    devices = range(lax.axis_size(axis))
    route = [(i, i ^ step) for i in devices if not (upward_only and i & step)]
    return lax.ppermute(block, axis, route)


def carried_in(log_total, state, axis):
    count, mine = lax.axis_size(axis), lax.axis_index(axis)
    heads, width = log_total.size, state.shape[-1]
    flat = state.reshape(heads, -1, width)
    decay = jnp.exp(log_total).reshape(heads)
    total, before, before_decay = flat, jnp.zeros_like(flat), jnp.ones_like(decay)
    step = 1
    while step < count:
        coarse = lax.reduce_precision(decay, 8, 7)
        lane = jnp.arange(width)[None, :]
        tail = jnp.where(lane == 0, coarse[:, None], jnp.where(lane == 1, (decay - coarse)[:, None], 0.0))
        sent = jnp.concatenate([total.reshape(-1, width), tail], axis=0).astype(jnp.bfloat16)
        got = swap(sent, axis, step, 2 * step >= count).astype(jnp.float32)
        other = got[: got.shape[0] - heads].reshape(flat.shape)
        other_decay = got[got.shape[0] - heads :, 0] + got[got.shape[0] - heads :, 1]
        upper = (mine & step) != 0
        before = before + jnp.where(upper, before_decay, 0.0)[:, None, None] * other
        if 2 * step < count:
            before_decay = before_decay * jnp.where(upper, other_decay, 1.0)
            total = jnp.where(
                upper, other * decay[:, None, None] + total, total * other_decay[:, None, None] + other
            )
            decay = decay * other_decay
        step *= 2
    return before.reshape(state.shape)


def causal_conv(previous, current, weight):
    stacked = jnp.concatenate([previous, current], axis=0).astype(jnp.float32)
    weight = weight.astype(jnp.float32)
    kernel_len = weight.shape[0]
    length = current.shape[0]
    summed_taps = weight[0] * stacked[0:length]
    for offset in range(1, kernel_len):
        summed_taps = summed_taps + weight[offset] * stacked[offset : offset + length]
    return jax.nn.silu(summed_taps)


def product(spec, *operands):
    return jnp.einsum(
        spec, *[part.astype(jnp.bfloat16) for part in operands], preferred_element_type=jnp.float32
    )


def on_device(
    stream,
    head_input_signal,
    write_input_vectors,
    read_input_vectors,
    output_gate_input,
    step_size_input,
    position_log_decay,
    signal_filter_taps,
    write_filter_taps,
    read_filter_taps,
    step_size_bias,
    head_decay_rate,
    head_direct_term,
    grouped_norm_gain,
    mixer_output_weight,
    expert_norm_gain,
    chosen_expert_index,
    chosen_expert_weight,
    routed_gate_weight,
    routed_up_weight,
    routed_down_weight,
    common_gate_weight,
    common_up_weight,
    common_down_weight,
):
    length = head_input_signal.shape[0]
    margin = signal_filter_taps.shape[0] - 1
    head_count = step_size_input.shape[1]
    groups = write_input_vectors.shape[1] // STATE
    per_group = head_count // groups
    blocks = length // BLK
    wide, narrow = head_input_signal.shape[1], write_input_vectors.shape[1]
    rim = jnp.concatenate(
        [part[length - margin :] for part in (head_input_signal, write_input_vectors, read_input_vectors)],
        axis=1,
    )
    rim = from_behind(rim, "sp", 1)
    before = (rim[:, :wide], rim[:, wide : wide + narrow], rim[:, wide + narrow :])
    signal = causal_conv(before[0], head_input_signal, signal_filter_taps)
    write_vec = causal_conv(before[1], write_input_vectors, write_filter_taps)
    read_vec = causal_conv(before[2], read_input_vectors, read_filter_taps)
    time_position = jax.nn.softplus(step_size_input.astype(jnp.float32) + step_size_bias)
    decay_logarithm = position_log_decay - head_decay_rate * time_position
    signal_heads = signal.reshape(blocks, BLK, groups, per_group, HEAD_DIM)
    scaled_blocks = signal_heads * time_position.reshape(blocks, BLK, groups, per_group)[..., None]
    write_blocks = write_vec.reshape(blocks, BLK, groups, STATE)
    read_blocks = read_vec.reshape(blocks, BLK, groups, STATE)
    within_cum = jnp.cumsum(decay_logarithm.reshape(blocks, BLK, groups, per_group), axis=1)
    block_total = within_cum[:, -1]
    running = jnp.cumsum(block_total, axis=0)
    device_total = running[-1]
    causal = jnp.arange(BLK)[:, None] >= jnp.arange(BLK)[None, :]
    cum_heads = jnp.transpose(within_cum, (0, 2, 3, 1))
    differences = cum_heads[..., :, None] - cum_heads[..., None, :]
    decay_matrix = jnp.exp(jnp.where(causal, differences, -jnp.inf))
    tail_decay = jnp.exp(block_total[:, None] - within_cum)
    block_states = product(
        "bsgn,bsgep->bgepn", write_blocks, scaled_blocks * tail_decay[..., None]
    )
    device_state = jnp.sum(
        block_states * jnp.exp(device_total[None] - running)[..., None, None], axis=0
    )
    incoming = carried_in(device_total, device_state, "sp")
    intersection = product("btgn,bsgn->bgts", read_blocks, write_blocks)
    intra_out = product(
        "bgets,bsgep->btgep", intersection[:, :, None] * decay_matrix, scaled_blocks
    )
    readout_scale = jnp.exp(within_cum)
    starts = [incoming]
    for block in range(blocks - 1):
        starts.append(
            starts[-1] * jnp.exp(block_total[block])[..., None, None] + block_states[block]
        )
    near_out = (
        product("btgn,bgepn->btgep", read_blocks, jnp.stack(starts)) * readout_scale[..., None]
    )
    ssd_out = intra_out + near_out
    ssd_out = ssd_out + head_direct_term.reshape(groups, per_group)[:, :, None] * signal_heads
    gated = ssd_out.reshape(length, groups, per_group * HEAD_DIM) * jax.nn.silu(
        output_gate_input.astype(jnp.float32)
    ).reshape(length, groups, per_group * HEAD_DIM)
    norm_scale = lax.rsqrt(jnp.mean(gated * gated, axis=-1, keepdims=True) + 1e-06)
    mixer_out = ((gated * norm_scale).reshape(length, -1) * grouped_norm_gain).astype(jnp.bfloat16)
    row_count = stream.shape[0]
    tp_count = lax.axis_size("tp")
    core = lax.axis_index("tp")

    def share_of(owner):
        rows = lax.dynamic_slice_in_dim(mixer_out, owner * row_count, row_count, 0)
        return jnp.dot(rows, mixer_output_weight, preferred_element_type=jnp.float32)

    shares = []
    for ahead in range(1, tp_count):
        route = [(i, (i + ahead) % tp_count) for i in range(tp_count)]
        part = share_of((core + ahead) % tp_count).astype(jnp.bfloat16)
        shares.append(lax.ppermute(part, "tp", route))
    summed = share_of(core)
    for part in shares:
        summed = summed + part.astype(jnp.float32)
    residual = (stream.astype(jnp.float32) + summed).astype(jnp.bfloat16)
    widened = residual.astype(jnp.float32)
    normed = (
        widened
        * lax.rsqrt(jnp.mean(widened * widened, axis=-1, keepdims=True) + 1e-06)
        * expert_norm_gain
    ).astype(jnp.bfloat16)
    shared_hidden = (
        jax.nn.silu(jnp.dot(normed, common_gate_weight, preferred_element_type=jnp.float32))
        * jnp.dot(normed, common_up_weight, preferred_element_type=jnp.float32)
    ).astype(jnp.bfloat16)
    shared = jnp.dot(shared_hidden, common_down_weight, preferred_element_type=jnp.float32)
    sp_count = lax.axis_size("sp")
    experts = sp_count * tp_count
    fanout = chosen_expert_index.shape[1]
    capacity = max(2, (3 * row_count * fanout + 2 * experts - 1) // (2 * experts))
    named = chosen_expert_index[:, :, None] == jnp.arange(experts, dtype=jnp.int32)
    hits = jnp.any(named, axis=1)
    share = jnp.sum(jnp.where(named, chosen_expert_weight[:, :, None], 0.0), axis=1)
    ahead = (jnp.arange(row_count)[:, None] > jnp.arange(row_count)[None, :]).astype(jnp.bfloat16)
    slot = jnp.dot(ahead, hits.astype(jnp.bfloat16), preferred_element_type=jnp.float32)
    slot = jnp.where(hits, slot.astype(jnp.int32), -1)
    places = jnp.arange(capacity, dtype=jnp.int32)
    half = experts // 2
    side = lax.axis_index("sp") // (sp_count // 2)
    sides = [list(range(half)), list(range(half, experts))]
    across = sp_count // 2
    tables = jnp.stack([slot.astype(jnp.float32), share])
    near_table = lax.dynamic_slice_in_dim(tables, side * half, half, 2)
    far_table = swap(
        lax.dynamic_slice_in_dim(tables, (1 - side) * half, half, 2), "sp", across, False
    )

    def exchange(block):
        return lax.all_to_all(
            block,
            ("sp", "tp"),
            split_axis=0,
            concat_axis=0,
            axis_index_groups=sides,
            tiled=True,
        )

    def dispatch(table, rows):
        slots = table[0].astype(jnp.int32)
        pick = slots.T[:, None, :] == places[None, :, None]
        pick = pick.reshape(half * capacity, row_count).astype(jnp.bfloat16)
        picked = jnp.dot(pick, rows, preferred_element_type=jnp.float32)
        return exchange(picked.astype(jnp.bfloat16).reshape(half, capacity, -1))

    def expert(arrived):
        flat_rows = arrived.reshape(half * capacity, -1)
        hidden = (
            jax.nn.silu(
                jnp.dot(flat_rows, routed_gate_weight[0], preferred_element_type=jnp.float32)
            )
            * jnp.dot(flat_rows, routed_up_weight[0], preferred_element_type=jnp.float32)
        ).astype(jnp.bfloat16)
        result = jnp.dot(hidden, routed_down_weight[0], preferred_element_type=jnp.float32)
        return result.astype(jnp.bfloat16).reshape(arrived.shape)

    def collect(table, returned):
        slots = table[0].astype(jnp.int32)
        spread = jnp.where(slots[:, :, None] == places, table[1][:, :, None], 0.0)
        spread = spread.reshape(row_count, half * capacity)
        coarse = lax.reduce_precision(spread, 8, 7)
        fine = (spread - coarse).astype(jnp.bfloat16)
        back = returned.reshape(half * capacity, -1)
        return jnp.dot(
            coarse.astype(jnp.bfloat16), back, preferred_element_type=jnp.float32
        ) + jnp.dot(fine, back, preferred_element_type=jnp.float32)

    far_rows = swap(normed, "sp", across, False)
    near_rows = dispatch(near_table, normed)
    near_rows, far_rows = lax.optimization_barrier((near_rows, far_rows))
    far_arrived = dispatch(far_table, far_rows)
    near_out = expert(near_rows)
    far_out = expert(far_arrived)
    far_sum = collect(far_table, exchange(far_out)).astype(jnp.bfloat16)
    near_out, far_sum = lax.optimization_barrier((near_out, far_sum))
    from_far = swap(far_sum, "sp", across, False)
    near_sum = collect(near_table, exchange(near_out))
    return (widened + shared + near_sum + from_far.astype(jnp.float32)).astype(jnp.bfloat16)


def solution(mesh):
    in_specs = (
        P(("sp", "tp"), None),
        P("sp", "tp"),
        P("sp", "tp"),
        P("sp", "tp"),
        P("sp", "tp"),
        P("sp", "tp"),
        P("sp", "tp"),
        P(None, "tp"),
        P(None, "tp"),
        P(None, "tp"),
        P("tp"),
        P("tp"),
        P("tp"),
        P("tp"),
        P("tp", None),
        P(),
        P(("sp", "tp"), None),
        P(("sp", "tp"), None),
        P(("sp", "tp"), None, None),
        P(("sp", "tp"), None, None),
        P(("sp", "tp"), None, None),
        P(),
        P(),
        P(),
    )
    out_specs = P(("sp", "tp"), None)
    return jax.shard_map(
        on_device, mesh=mesh, in_specs=in_specs, out_specs=out_specs, check_vma=False
    )
```
